512 devices in a mesh: sp: 128 (over z, y, core), tp: 4 (over x).
Axes of the slice: x: 4, y: 8, z: 8, core: 2. Of those that a mesh axis runs over, the one named last changes fastest.
Arguments:
- tokens: bfloat16 [65536, 2048], P('sp'), may hold values from -24 to 24
- w_query: bfloat16 [2048, 1536], P('sp', 'tp'), as said below
- w_key: bfloat16 [2048, 1536], P('sp', 'tp'), as said below
- w_value: bfloat16 [2048, 1536], P('sp', 'tp'), may hold values from -0.125 to 0.125
- w_out: bfloat16 [512, 2048], P('tp', 'sp'), may hold values from -1.5 to 1.5
Outputs:
- mixed: bfloat16 [65536, 2048], P(('sp', 'tp'))
The draws below stay inside these ranges and needn't reach their ends.
Inputs may be any that keep to these rules, and one draw needn't show every extreme that they name: `w_query`: every entry lies within 4 / sqrt(2048) of zero. `w_key`: every entry lies within 4 / sqrt(2048) of zero.
All inputs are finite; a program needn't handle non-finite values.
Results may differ from the reference program's by a relative error of at most 0.025.
Values may be sent and summed in bfloat16 or wider, within the bound.
No kernel may reach another device: no remote copies, remote signals or barrier semaphores. Data moves between devices by JAX's collectives and lax.ppermute only.
A program may use at most 64 MiB of HBM per device.

```python
import math
import jax
import jax.numpy as jnp
from jax import lax

D = 2048
HEADS = 4
GROUPS = 3
DH = 128
WIN1 = 128
WIN2 = 512
WIN3 = 2048
SECOND_DILATION = 4
THIRD_DILATION = 16
SEQ = 65536


def shared_query(key):
    return jax.random.normal(jax.random.fold_in(key, 101), (D, HEADS * GROUPS * DH), jnp.float32)


def draw_tokens(key, part):
    drawn = jax.random.normal(jax.random.fold_in(key, 1), (SEQ, D), jnp.float32)
    return jnp.clip(drawn, -24.0, 24.0).astype(jnp.bfloat16)


def draw_w_query(key, part):
    limit = 4.0 * D ** (-0.5)
    return jnp.clip(shared_query(key) * D ** (-0.5), -limit, limit).astype(jnp.bfloat16)


def draw_w_key(key, part):
    limit = 4.0 * D ** (-0.5)
    own_part = jax.random.normal(jax.random.fold_in(key, 202), (D, HEADS * GROUPS * DH), jnp.float32)
    return jnp.clip(own_part * D ** (-0.5), -limit, limit).astype(jnp.bfloat16)


def shard_levels(own_key, shape, cuts, smallest, top_value):
    level, own = 1.0, jax.random.fold_in(own_key, 6)
    for axis_at, blocks in cuts:
        steps = jnp.exp(jax.random.uniform(jax.random.fold_in(own, axis_at), (blocks,), jnp.float32, smallest / len(cuts), top_value / len(cuts)))
        level = level * jnp.repeat(steps, shape[axis_at] // blocks).reshape([-1 if axis == axis_at else 1 for axis in range(len(shape))])
    return level


def scatter_about(own_key, dims, scale, bound, cuts=(), kind=jnp.bfloat16):
    loudness = shard_levels(own_key, dims, cuts, -0.22, 0.18) if cuts else 1.0
    drawn = jax.random.normal(own_key, dims, jnp.float32) * scale * loudness
    return jnp.minimum(jnp.maximum(drawn, -bound), bound).astype(kind)


def setup_inputs(seed: int = 0) -> dict:
    arg_keys = jax.random.split(jax.random.key(seed), 6)
    tokens = draw_tokens(jax.random.fold_in(arg_keys[5], 71), 0)
    w_query = draw_w_query(jax.random.fold_in(arg_keys[5], 71), 0)
    w_key = draw_w_key(jax.random.fold_in(arg_keys[5], 71), 0)
    w_value = scatter_about(arg_keys[3], (D, HEADS * GROUPS * DH), D ** -0.5, 0.125, ((0, 128), (1, 4)))
    w_out = scatter_about(arg_keys[4], (HEADS * DH, D), 0.35, 1.5, ((0, 4), (1, 128)))
    return dict(tokens=tokens, w_query=w_query, w_key=w_key, w_value=w_value, w_out=w_out)


ROPE_BASE = 500000.0


def rotate(projected):
    seq_len = projected.shape[0]
    head_size = projected.shape[-1]
    half_size = head_size // 2
    positions = jnp.arange(seq_len, dtype=jnp.int32).astype(jnp.float32)
    frequency = 1.0 / (ROPE_BASE ** (jnp.arange(0, head_size, 2, dtype=jnp.float32) / head_size))
    angles = (positions[:, None] * frequency[None, :]).reshape(seq_len, 1, 1, half_size)
    cosine = jnp.cos(angles)
    sine_part = jnp.sin(angles)
    first_half = projected[..., :half_size]
    second_half = projected[..., half_size:]
    return jnp.concatenate([first_half * cosine - second_half * sine_part,
                            second_half * cosine + first_half * sine_part], axis=-1)


def window_attend(queries, keys, values, window, stride):
    seq_len, heads, head_size = queries.shape
    block_rows = math.gcd(seq_len, 512)
    block_list = seq_len // block_rows
    key_pad = jnp.pad(keys, ((window, 0), (0, 0), (0, 0)))
    value_pad = jnp.pad(values, ((window, 0), (0, 0), (0, 0)))
    query_blocks = queries.reshape(block_list, block_rows, heads, head_size)

    def one_block(operands):
        query_block, block_index = operands
        begin = (block_index * block_rows).astype(jnp.int32)
        key_slab = lax.dynamic_slice_in_dim(key_pad, begin, block_rows + window, 0)
        value_band = lax.dynamic_slice_in_dim(value_pad, begin, block_rows + window, 0)
        scores = jnp.einsum('qhe,khe->hqk', query_block.astype(jnp.float32),
                            key_slab.astype(jnp.float32)) * (head_size ** -0.5)
        query_pos = begin + jnp.arange(block_rows, dtype=jnp.int32)
        key_pos = begin - window + jnp.arange(block_rows + window, dtype=jnp.int32)
        spacing = query_pos[:, None] - key_pos[None, :]
        allowed = (spacing >= 0) & (spacing <= window) & (spacing % stride == 0) & (key_pos[None, :] >= 0)
        scores = jnp.where(allowed[None], scores, -jnp.inf)
        row_max = jnp.max(scores, axis=-1)
        exponent = jnp.exp(scores - row_max[..., None])
        totals = jnp.sum(exponent, axis=-1)
        probs = lax.optimization_barrier((exponent / totals[..., None]).astype(jnp.bfloat16))
        mixed = jnp.einsum('hqk,khe->qhe', probs.astype(jnp.float32), value_band.astype(jnp.float32))
        return mixed, jnp.transpose(row_max + jnp.log(totals))

    mixed, log_totals = lax.map(one_block, (query_blocks, jnp.arange(block_list, dtype=jnp.int32)))
    return mixed.reshape(seq_len, heads, head_size), log_totals.reshape(seq_len, heads)


def reference(tokens, w_query, w_key, w_value, w_out):
    seq_len = tokens.shape[0]
    head_shape = (seq_len, HEADS, GROUPS, DH)
    query_raw = jnp.dot(tokens, w_query, preferred_element_type=jnp.float32).reshape(head_shape)
    key_raw = jnp.dot(tokens, w_key, preferred_element_type=jnp.float32).reshape(head_shape)
    values = lax.optimization_barrier(
        jnp.dot(tokens, w_value, preferred_element_type=jnp.float32).astype(jnp.bfloat16)).reshape(head_shape)
    queries = lax.optimization_barrier(rotate(query_raw).astype(jnp.bfloat16))
    keys = lax.optimization_barrier(rotate(key_raw).astype(jnp.bfloat16))
    windows = (WIN1, WIN2, WIN3)
    step_sizes = (1, SECOND_DILATION, THIRD_DILATION)
    outputs = []
    log_totals = []
    for group_index in range(GROUPS):
        group_out, log_total = window_attend(queries[:, :, group_index], keys[:, :, group_index],
                                             values[:, :, group_index], windows[group_index],
                                             step_sizes[group_index])
        outputs.append(group_out)
        log_totals.append(log_total)
    group_weights = jax.nn.softmax(jnp.stack(log_totals), axis=0)
    merged = jnp.sum(group_weights[..., None] * jnp.stack(outputs), axis=0).astype(jnp.bfloat16)
    merged = merged.reshape(seq_len, HEADS * DH)
    return jnp.dot(merged, w_out, preferred_element_type=jnp.float32).astype(jnp.bfloat16)
```

```python
import functools

import jax
import jax.numpy as jnp
from jax import lax
from jax.experimental import pallas as pl
from jax.experimental.pallas import tpu as pltpu
from jax.sharding import Mesh
from jax.sharding import PartitionSpec as P

DH = 128
ROWS = 512
ROPE_BASE = 500000.0
SP = ("z", "y", "core")
F32 = jnp.float32
BF16 = jnp.bfloat16
SCALE = DH ** (-0.5)
MIB = 1024 * 1024


def spread(value, axis):
    copies = jnp.broadcast_to(value, (lax.axis_size(axis), *value.shape))
    return lax.all_to_all(copies, axis, split_axis=0, concat_axis=0, tiled=True)


def from_behind(block, distance):
    size = lax.axis_size(SP)
    return lax.ppermute(block, SP, [(i - distance, i) for i in range(distance, size)])


def from_partner(block):
    return lax.ppermute(block, "core", [(0, 1), (1, 0)])


def call(body, outs, scratch=(), flops=0, moved=0, name=None, in_specs=None):
    extra = {} if in_specs is None else {"in_specs": in_specs}
    return pl.pallas_call(
        body,
        out_shape=outs,
        scratch_shapes=list(scratch),
        compiler_params=pltpu.CompilerParams(vmem_limit_bytes=48 * MIB),
        cost_estimate=pl.CostEstimate(flops=flops, bytes_accessed=moved, transcendentals=0),
        name=name,
        **extra,
    )


def tables(offset):
    positions = (offset + jnp.arange(ROWS, dtype=jnp.int32)).astype(F32)
    frequency = 1.0 / ROPE_BASE ** (jnp.arange(0, DH, 2, dtype=F32) / DH)
    angles = positions[:, None] * frequency[None, :]
    cosine, sine = jnp.cos(angles), jnp.sin(angles)
    return jnp.concatenate([cosine, cosine], axis=1), jnp.concatenate([-sine, sine], axis=1)


def turned(raw, cos_ref, sin_ref):
    return raw * cos_ref[...] + pltpu.roll(raw, DH // 2, 1) * sin_ref[...]


def reorder_body(tok_ref, out_ref):
    row = lax.broadcasted_iota(jnp.int32, (256, 256), 0)
    col = lax.broadcasted_iota(jnp.int32, (256, 256), 1)
    target = ((row >> 4) & 1) * 128 + (row >> 5) * 16 + (row & 15)
    moves = (col == target).astype(BF16)
    for z in range(8):
        part = tok_ref[:, z * 256 : (z + 1) * 256]
        out_ref[:, z * 256 : (z + 1) * 256] = jnp.dot(part, moves, preferred_element_type=F32).astype(BF16)


def by_residue(value, stage_ref, out_ref, base, stride):
    stage_ref[...] = value
    count = ROWS // stride
    for r in range(stride):
        out_ref[base + r * count : base + (r + 1) * count, :] = stage_ref[
            pl.ds(r, count, stride=stride), :
        ].astype(BF16)


def kv3_body(tok_ref, w_ref, cos_ref, sin_ref, out_ref, stage_ref):
    acc = jnp.zeros((ROWS, 2 * DH), F32)
    for z in range(8):
        rows = jnp.concatenate([w_ref[0, z], w_ref[1, z]], axis=0)
        acc = acc + jnp.dot(tok_ref[:, z * 256 : (z + 1) * 256], rows, preferred_element_type=F32)
    by_residue(turned(acc[:, :DH], cos_ref, sin_ref), stage_ref, out_ref, 0, 16)
    by_residue(acc[:, DH:], stage_ref, out_ref, ROWS, 16)


def kv12_body(tok_ref, w_ref, cos_ref, sin_ref, own_ref, send_ref, stage_ref):
    keys = jnp.dot(tok_ref[...], w_ref[:, : 2 * DH], preferred_element_type=F32)
    near = turned(keys[:, :DH], cos_ref, sin_ref).astype(BF16)
    own_ref[:ROWS] = near
    send_ref[:128] = near[ROWS - 128 :]
    by_residue(turned(keys[:, DH:], cos_ref, sin_ref), stage_ref, send_ref, 256, 4)
    values = jnp.dot(tok_ref[...], w_ref[:, 2 * DH :], preferred_element_type=F32)
    near = values[:, :DH].astype(BF16)
    own_ref[ROWS:] = near
    send_ref[128:256] = near[ROWS - 128 :]
    by_residue(values[:, DH:], stage_ref, send_ref, 256 + ROWS, 4)


def attend(query, key, value, allowed):
    scores = lax.dot_general(query, key, (((1,), (1,)), ((), ())), preferred_element_type=F32) * SCALE
    scores = jnp.where(allowed, scores, -jnp.inf)
    top = jnp.max(scores, axis=-1, keepdims=True)
    weight = jnp.exp(scores - top)
    total = jnp.sum(weight, axis=-1, keepdims=True)
    probs = (weight * (1.0 / total)).astype(BF16)
    return jnp.dot(probs, value, preferred_element_type=F32), top + jnp.log(total)


def q_body(spi_ref, tok_ref, w_ref, cos_ref, sin_ref, x4, x3, x2, x1, x0, q_ref, out_ref, log_ref, stage_ref, q3_ref):
    spi = spi_ref[0, 0]
    first = jnp.dot(tok_ref[...], w_ref[:, : 2 * DH], preferred_element_type=F32)
    q_ref[:ROWS] = turned(first[:, :DH], cos_ref, sin_ref).astype(BF16)
    by_residue(turned(first[:, DH:], cos_ref, sin_ref), stage_ref, q_ref, ROWS, 4)
    third = jnp.dot(tok_ref[...], w_ref[:, 2 * DH : 3 * DH], preferred_element_type=F32)
    by_residue(turned(third, cos_ref, sin_ref), stage_ref, q3_ref, 0, 16)
    row = lax.broadcasted_iota(jnp.int32, (32, 160), 0)
    col = lax.broadcasted_iota(jnp.int32, (32, 160), 1)
    back = row + 128 - col
    allowed = (back >= 0) & (back <= 128) & ((col >> 5) + spi >= 4)
    for r in range(16):
        at = slice(r * 32, (r + 1) * 32)
        later = slice(ROWS + r * 32, ROWS + (r + 1) * 32)
        key = jnp.concatenate([x[at] for x in (x4, x3, x2, x1, x0)], axis=0)
        value = jnp.concatenate([x[later] for x in (x4, x3, x2, x1, x0)], axis=0)
        out, log_total = attend(q3_ref[at], key, value, allowed)
        out_ref[pl.ds(r, 32, stride=16), :] = out
        log_ref[pl.ds(r, 32, stride=16), :] = jnp.broadcast_to(log_total, (32, DH))


def merge_body(spi_ref, q_ref, own_ref, send_ref, halo_ref, out3_ref, log3_ref, merged_ref, out2, log2, out1, log1):
    spi = spi_ref[0, 0]
    row = lax.broadcasted_iota(jnp.int32, (128, 256), 0)
    col = lax.broadcasted_iota(jnp.int32, (128, 256), 1)
    back = row + 128 - col
    inside = (back >= 0) & (back <= 128)
    edge = inside & ((col >= 128) | (spi >= 1))
    for r in range(4):
        at = slice(256 + r * 128, 256 + (r + 1) * 128)
        later = slice(256 + ROWS + r * 128, 256 + ROWS + (r + 1) * 128)
        key = jnp.concatenate([halo_ref[at], send_ref[at]], axis=0)
        value = jnp.concatenate([halo_ref[later], send_ref[later]], axis=0)
        out, log_total = attend(q_ref[ROWS + r * 128 : ROWS + (r + 1) * 128], key, value, edge)
        out2[pl.ds(r, 128, stride=4), :] = out
        log2[pl.ds(r, 128, stride=4), :] = jnp.broadcast_to(log_total, (128, DH))
    for b in range(4):
        if b == 0:
            key = jnp.concatenate([halo_ref[:128], own_ref[:128]], axis=0)
            value = jnp.concatenate([halo_ref[128:256], own_ref[ROWS : ROWS + 128]], axis=0)
        else:
            key = own_ref[(b - 1) * 128 : (b + 1) * 128]
            value = own_ref[ROWS + (b - 1) * 128 : ROWS + (b + 1) * 128]
        at = slice(b * 128, (b + 1) * 128)
        out, log_total = attend(q_ref[at], key, value, edge if b == 0 else inside)
        l1 = jnp.broadcast_to(log_total, (128, DH))
        out1[at] = out
        log1[at] = l1
    for b in range(4):
        at = slice(b * 128, (b + 1) * 128)
        l1, l2, l3 = log1[at], log2[at], log3_ref[at]
        top = jnp.maximum(jnp.maximum(l1, l2), l3)
        e1, e2, e3 = jnp.exp(l1 - top), jnp.exp(l2 - top), jnp.exp(l3 - top)
        merged = (e1 * out1[at] + e2 * out2[at] + e3 * out3_ref[at]) / (e1 + e2 + e3)
        merged_ref[at] = merged.astype(BF16)


def out_body(m_ref, w_ref, out_ref):
    left = jnp.concatenate([m_ref[h] for h in range(4)], axis=1)
    for z in range(8):
        heads = []
        for h in range(4):
            pieces = [
                w_ref[h, z * 256 + c * 128 + y * 16 : z * 256 + c * 128 + y * 16 + 16, :]
                for y in range(8)
                for c in range(2)
            ]
            heads.append(jnp.concatenate(pieces, axis=0))
        right = jnp.concatenate(heads, axis=1)
        out_ref[:, z * 256 : (z + 1) * 256] = lax.dot_general(
            left, right, (((1,), (1,)), ((), ())), preferred_element_type=F32
        ).astype(BF16)


def shape(rows, cols, dtype=BF16):
    return jax.ShapeDtypeStruct((rows, cols), dtype)


def on_device(tokens, w_query, w_key, w_value, w_out):
    spi = lax.axis_index(SP).astype(jnp.int32)
    core = lax.axis_index("core")
    vmem = pl.BlockSpec(memory_space=pltpu.VMEM)
    smem = pl.BlockSpec(memory_space=pltpu.SMEM)
    stage = pltpu.VMEM((ROWS, DH), F32)

    packed = jnp.concatenate(
        [w_key[:, :256], w_value[:, :256], w_query, w_out.T, w_key[:, 256:], w_value[:, 256:]], axis=1
    )
    line = spread(packed, "y").reshape(128, 1280)
    plane = lax.all_gather(line[:, :1024], ("z", "core"), axis=0, tiled=True)
    third = spread(spread(line[:, 1024:], "z"), "core")

    cos, sin = tables(spi * ROWS)
    tok = call(reorder_body, shape(ROWS, 2048), flops=2 * ROWS * 2048 * 256, moved=4 * MIB, name="reorder")(tokens)

    x0 = call(
        kv3_body, shape(2 * ROWS, DH), [stage], 2 * ROWS * 2048 * 256, 4 * MIB, "kv3"
    )(tok, third, cos, sin)
    x2 = from_behind(x0, 2)
    x4 = from_behind(x2, 2)
    x1 = from_partner(jnp.where(core == 0, x0, x2))
    x3 = from_partner(jnp.where(core == 0, x2, x4))

    own, send = call(
        kv12_body,
        (shape(2 * ROWS, DH), shape(1280, DH)),
        [stage],
        2 * ROWS * 2048 * 512,
        5 * MIB,
        "kv12",
    )(tok, plane[:, :512], cos, sin)
    halo = from_behind(send, 1)
    spi_cell = spi.reshape(1, 1)
    queries, out3, log3 = call(
        q_body,
        (shape(2 * ROWS, DH), shape(ROWS, DH, F32), shape(ROWS, DH, F32)),
        [stage, pltpu.VMEM((ROWS, DH), BF16)],
        2 * ROWS * 2048 * 384,
        6 * MIB,
        "q",
        [smem] + [vmem] * 9,
    )(spi_cell, tok, plane[:, 512:896], cos, sin, x4, x3, x2, x1, x0)
    merged = call(
        merge_body,
        shape(ROWS, DH),
        [stage] * 4,
        8 * 4 * 128 * 256 * 128,
        3 * MIB,
        "merge",
        [smem] + [vmem] * 6,
    )(spi_cell, queries, own, send, halo, out3, log3)

    all_heads = spread(plane[:, 896:], "tp")
    by_position = lax.all_to_all(merged.reshape(4, 128, DH), "tp", split_axis=0, concat_axis=0, tiled=True)
    return call(out_body, shape(128, 2048), flops=2 * 128 * 512 * 2048, moved=3 * MIB, name="project")(
        by_position, all_heads
    )


def solution(mesh):
    grid = Mesh(mesh.devices.reshape(8, 8, 2, 4), (*SP, "tp"))
    placed = (P(SP, None), P(SP, "tp"), P(SP, "tp"), P(SP, "tp"), P("tp", SP))
    return jax.shard_map(
        on_device, mesh=grid, in_specs=placed, out_specs=P((*SP, "tp"), None), check_vma=False
    )
```

```python
import jax
import jax.numpy as jnp
from jax import lax
from jax.experimental import pallas as pl
from jax.experimental.pallas import tpu as pltpu
from jax.sharding import Mesh
from jax.sharding import PartitionSpec as P

DH = 128
ROWS = 512
ROPE_BASE = 500000.0
SP = ("z", "y", "core")
F32 = jnp.float32
BF16 = jnp.bfloat16
SCALE = DH ** (-0.5)
MIB = 1024 * 1024


def spread(value, axis):
    copies = jnp.broadcast_to(value, (lax.axis_size(axis), *value.shape))
    return lax.all_to_all(copies, axis, split_axis=0, concat_axis=0, tiled=True)


def from_behind(block, distance):
    size = lax.axis_size(SP)
    return lax.ppermute(block, SP, [(i - distance, i) for i in range(distance, size)])


def from_partner(block):
    return lax.ppermute(block, "core", [(0, 1), (1, 0)])


def call(body, outs, scratch=(), flops=0, moved=0, name=None, in_specs=None):
    extra = {} if in_specs is None else {"in_specs": in_specs}
    return pl.pallas_call(
        body,
        out_shape=outs,
        scratch_shapes=list(scratch),
        compiler_params=pltpu.CompilerParams(vmem_limit_bytes=24 * MIB),
        cost_estimate=pl.CostEstimate(flops=flops, bytes_accessed=moved, transcendentals=0),
        name=name,
        **extra,
    )


def tables(offset):
    positions = (offset + jnp.arange(ROWS, dtype=jnp.int32)).astype(F32)
    frequency = 1.0 / ROPE_BASE ** (jnp.arange(0, DH, 2, dtype=F32) / DH)
    angles = positions[:, None] * frequency[None, :]
    cosine, sine = jnp.cos(angles), jnp.sin(angles)
    return jnp.concatenate([cosine, cosine], axis=1), jnp.concatenate([-sine, sine], axis=1)


def turned(raw, cos_ref, sin_ref):
    return raw * cos_ref[...] + pltpu.roll(raw, DH // 2, 1) * sin_ref[...]


def reorder_body(tok_ref, out_ref):
    row = lax.broadcasted_iota(jnp.int32, (256, 256), 0)
    col = lax.broadcasted_iota(jnp.int32, (256, 256), 1)
    target = ((row >> 4) & 1) * 128 + (row >> 5) * 16 + (row & 15)
    moves = (col == target).astype(BF16)
    for z in range(8):
        part = tok_ref[:, z * 256 : (z + 1) * 256]
        out_ref[:, z * 256 : (z + 1) * 256] = jnp.dot(part, moves, preferred_element_type=F32).astype(BF16)


def pack_body(q_ref, k_ref, v_ref, o_ref, out_ref):
    for y in range(8):
        out_ref[y, :, 0:256] = k_ref[:, :256]
        out_ref[y, :, 256:512] = v_ref[:, :256]
        for h in range(4):
            out_ref[y, :, 512 + h * DH : 512 + (h + 1) * DH] = o_ref[h]
        out_ref[y, :, 1024:1408] = q_ref[...]
        out_ref[y, :, 1408:1536] = k_ref[:, 256:]
        out_ref[y, :, 1536:1664] = v_ref[:, 256:]


def unpack_body(line_ref, most_ref, third_ref):
    for y in range(8):
        at = slice(y * 16, (y + 1) * 16)
        most_ref[at] = line_ref[y, :, :1408]
        for z in range(8):
            third_ref[z, at] = line_ref[y, :, 1408:]


def by_residue(value, stage_ref, out_ref, base, stride):
    stage_ref[...] = value
    count = ROWS // stride
    for r in range(stride):
        out_ref[base + r * count : base + (r + 1) * count, :] = stage_ref[
            pl.ds(r, count, stride=stride), :
        ].astype(BF16)


def kv3_body(tok_ref, w_ref, cos_ref, sin_ref, out_ref, stage_ref):
    acc = jnp.zeros((ROWS, 2 * DH), F32)
    for z in range(8):
        rows = jnp.concatenate([w_ref[0, z], w_ref[1, z]], axis=0)
        acc = acc + jnp.dot(tok_ref[:, z * 256 : (z + 1) * 256], rows, preferred_element_type=F32)
    by_residue(turned(acc[:, :DH], cos_ref, sin_ref), stage_ref, out_ref, 0, 16)
    by_residue(acc[:, DH:], stage_ref, out_ref, ROWS, 16)


def kv12_body(tok_ref, plane_ref, cos_ref, sin_ref, own_ref, send_ref, stage_ref, w_ref, key_sem, value_sem):
    key_copy = pltpu.make_async_copy(plane_ref.at[:, : 2 * DH], w_ref.at[:, : 2 * DH], key_sem)
    value_copy = pltpu.make_async_copy(plane_ref.at[:, 2 * DH : 4 * DH], w_ref.at[:, 2 * DH :], value_sem)
    key_copy.start()
    value_copy.start()
    key_copy.wait()
    keys = jnp.dot(tok_ref[...], w_ref[:, : 2 * DH], preferred_element_type=F32)
    near = turned(keys[:, :DH], cos_ref, sin_ref).astype(BF16)
    own_ref[:ROWS] = near
    send_ref[:128] = near[ROWS - 128 :]
    by_residue(turned(keys[:, DH:], cos_ref, sin_ref), stage_ref, send_ref, 256, 4)
    value_copy.wait()
    values = jnp.dot(tok_ref[...], w_ref[:, 2 * DH :], preferred_element_type=F32)
    near = values[:, :DH].astype(BF16)
    own_ref[ROWS:] = near
    send_ref[128:256] = near[ROWS - 128 :]
    by_residue(values[:, DH:], stage_ref, send_ref, 256 + ROWS, 4)


def product(query, key):
    return lax.dot_general(query, key, (((1,), (1,)), ((), ())), preferred_element_type=F32)


def shares(scores, allowed):
    scores = jnp.where(allowed, scores * SCALE, -jnp.inf)
    top = jnp.max(scores, axis=-1, keepdims=True)
    weight = jnp.exp(scores - top)
    total = jnp.sum(weight, axis=-1, keepdims=True)
    return (weight * (1.0 / total)).astype(BF16), top + jnp.log(total)


def attend(query, key, value, allowed):
    probs, log_total = shares(product(query, key), allowed)
    return jnp.dot(probs, value, preferred_element_type=F32), log_total


def q_body(
    spi_ref, tok_ref, plane_ref, cos_ref, sin_ref, x4, x3, x2, x1, x0, q_ref, out_ref, log_ref,
    stage_ref, q3_ref, w_ref, first_sem, third_sem,
):
    third_copy = pltpu.make_async_copy(plane_ref.at[:, 1280:1408], w_ref.at[:, 256:], third_sem)
    first_copy = pltpu.make_async_copy(plane_ref.at[:, 1024:1280], w_ref.at[:, :256], first_sem)
    third_copy.start()
    first_copy.start()
    spi = spi_ref[0, 0]
    third_copy.wait()
    third = jnp.dot(tok_ref[...], w_ref[:, 256:], preferred_element_type=F32)
    by_residue(turned(third, cos_ref, sin_ref), stage_ref, q3_ref, 0, 16)
    first_copy.wait()
    first = jnp.dot(tok_ref[...], w_ref[:, :256], preferred_element_type=F32)
    q_ref[:ROWS] = turned(first[:, :DH], cos_ref, sin_ref).astype(BF16)
    by_residue(turned(first[:, DH:], cos_ref, sin_ref), stage_ref, q_ref, ROWS, 4)
    row = lax.broadcasted_iota(jnp.int32, (ROWS, 160), 0) & 31
    col = lax.broadcasted_iota(jnp.int32, (ROWS, 160), 1)
    back = row + 128 - col
    allowed = (back >= 0) & (back <= 128) & ((col >> 5) + spi >= 4)
    scores = []
    for r in range(16):
        at = slice(r * 32, (r + 1) * 32)
        key = jnp.concatenate([x[at] for x in (x4, x3, x2, x1, x0)], axis=0)
        scores.append(product(q3_ref[at], key))
    probs, log_total = shares(jnp.concatenate(scores, axis=0), allowed)
    wide = jnp.broadcast_to(log_total, (ROWS, DH))
    outs = []
    for r in range(16):
        later = slice(ROWS + r * 32, ROWS + (r + 1) * 32)
        value = jnp.concatenate([x[later] for x in (x4, x3, x2, x1, x0)], axis=0)
        outs.append(jnp.dot(probs[r * 32 : (r + 1) * 32], value, preferred_element_type=F32))
    for r in range(16):
        out_ref[pl.ds(r, 32, stride=16), :] = outs[r]
        log_ref[pl.ds(r, 32, stride=16), :] = wide[r * 32 : (r + 1) * 32]


def merge_body(spi_ref, q_ref, own_ref, send_ref, halo_ref, out3_ref, log3_ref, merged_ref, out2, log2, out1, log1):
    spi = spi_ref[0, 0]
    row = lax.broadcasted_iota(jnp.int32, (128, 256), 0)
    col = lax.broadcasted_iota(jnp.int32, (128, 256), 1)
    back = row + 128 - col
    inside = (back >= 0) & (back <= 128)
    edge = inside & ((col >= 128) | (spi >= 1))
    for r in range(4):
        at = slice(256 + r * 128, 256 + (r + 1) * 128)
        later = slice(256 + ROWS + r * 128, 256 + ROWS + (r + 1) * 128)
        key = jnp.concatenate([halo_ref[at], send_ref[at]], axis=0)
        value = jnp.concatenate([halo_ref[later], send_ref[later]], axis=0)
        out, log_total = attend(q_ref[ROWS + r * 128 : ROWS + (r + 1) * 128], key, value, edge)
        out2[pl.ds(r, 128, stride=4), :] = out
        log2[pl.ds(r, 128, stride=4), :] = jnp.broadcast_to(log_total, (128, DH))
    for b in range(4):
        if b == 0:
            key = jnp.concatenate([halo_ref[:128], own_ref[:128]], axis=0)
            value = jnp.concatenate([halo_ref[128:256], own_ref[ROWS : ROWS + 128]], axis=0)
        else:
            key = own_ref[(b - 1) * 128 : (b + 1) * 128]
            value = own_ref[ROWS + (b - 1) * 128 : ROWS + (b + 1) * 128]
        at = slice(b * 128, (b + 1) * 128)
        out, log_total = attend(q_ref[at], key, value, edge if b == 0 else inside)
        l1 = jnp.broadcast_to(log_total, (128, DH))
        out1[at] = out
        log1[at] = l1
    for b in range(4):
        at = slice(b * 128, (b + 1) * 128)
        l1, l2, l3 = log1[at], log2[at], log3_ref[at]
        top = jnp.maximum(jnp.maximum(l1, l2), l3)
        e1, e2, e3 = jnp.exp(l1 - top), jnp.exp(l2 - top), jnp.exp(l3 - top)
        merged = (e1 * out1[at] + e2 * out2[at] + e3 * out3_ref[at]) / (e1 + e2 + e3)
        merged_ref[at] = merged.astype(BF16)


def out_body(m_ref, plane_ref, out_ref, w_ref, sem):
    copy = pltpu.make_async_copy(plane_ref.at[:, 512:1024], w_ref, sem)
    copy.start()
    left = jnp.concatenate([m_ref[h] for h in range(4)], axis=1)
    copy.wait()
    for z in range(8):
        pieces = []
        for y in range(8):
            for c in range(2):
                start = z * 256 + c * 128 + y * 16
                pieces.append(w_ref[start : start + 16, :])
        right = jnp.concatenate(pieces, axis=0)
        out_ref[:, z * 256 : (z + 1) * 256] = product(left, right).astype(BF16)


def shape(rows, cols, dtype=BF16):
    return jax.ShapeDtypeStruct((rows, cols), dtype)


def on_device(tokens, w_query, w_key, w_value, w_out):
    spi = lax.axis_index(SP).astype(jnp.int32)
    core = lax.axis_index("core")
    vmem = pl.BlockSpec(memory_space=pltpu.VMEM)
    smem = pl.BlockSpec(memory_space=pltpu.SMEM)
    anywhere = pl.BlockSpec(memory_space=pltpu.HBM)
    dma = pltpu.SemaphoreType.DMA
    stage = pltpu.VMEM((ROWS, DH), F32)

    heads = spread(w_out.T, "tp")
    packed = call(pack_body, jax.ShapeDtypeStruct((8, 16, 1664), BF16), moved=MIB, name="pack")(
        w_query, w_key, w_value, heads
    )
    line = lax.all_to_all(packed, "y", split_axis=0, concat_axis=0, tiled=True)
    most, third = call(
        unpack_body, (shape(128, 1408), jax.ShapeDtypeStruct((8, 128, 256), BF16)), moved=MIB, name="unpack"
    )(line)
    plane = lax.all_gather(most, ("z", "core"), axis=0, tiled=True)
    third = spread(lax.all_to_all(third, "z", split_axis=0, concat_axis=0, tiled=True), "core")

    cos, sin = tables(spi * ROWS)
    tok = call(reorder_body, shape(ROWS, 2048), flops=2 * ROWS * 2048 * 256, moved=4 * MIB, name="reorder")(tokens)

    x0 = call(
        kv3_body, shape(2 * ROWS, DH), [stage], 2 * ROWS * 2048 * 256, 4 * MIB, "kv3"
    )(tok, third, cos, sin)
    x2 = from_behind(x0, 2)
    x4 = from_behind(x2, 2)
    x1 = from_partner(jnp.where(core == 0, x0, x2))
    x3 = from_partner(jnp.where(core == 0, x2, x4))

    own, send = call(
        kv12_body,
        (shape(2 * ROWS, DH), shape(1280, DH)),
        [stage, pltpu.VMEM((2048, 512), BF16), dma, dma],
        2 * ROWS * 2048 * 512,
        5 * MIB,
        "kv12",
        [vmem, anywhere, vmem, vmem],
    )(tok, plane, cos, sin)
    halo = from_behind(send, 1)
    spi_cell = spi.reshape(1, 1)
    queries, out3, log3 = call(
        q_body,
        (shape(2 * ROWS, DH), shape(ROWS, DH, F32), shape(ROWS, DH, F32)),
        [stage, pltpu.VMEM((ROWS, DH), BF16), pltpu.VMEM((2048, 384), BF16), dma, dma],
        2 * ROWS * 2048 * 384,
        6 * MIB,
        "q",
        [smem, vmem, anywhere] + [vmem] * 7,
    )(spi_cell, tok, plane, cos, sin, x4, x3, x2, x1, x0)
    merged = call(
        merge_body,
        shape(ROWS, DH),
        [stage] * 4,
        8 * 4 * 128 * 256 * 128,
        3 * MIB,
        "merge",
        [smem] + [vmem] * 6,
    )(spi_cell, queries, own, send, halo, out3, log3)

    by_position = lax.all_to_all(merged.reshape(4, 128, DH), "tp", split_axis=0, concat_axis=0, tiled=True)
    return call(
        out_body,
        shape(128, 2048),
        [pltpu.VMEM((2048, 512), BF16), dma],
        2 * 128 * 512 * 2048,
        3 * MIB,
        "project",
        [vmem, anywhere],
    )(by_position, plane)


def solution(mesh):
    grid = Mesh(mesh.devices.reshape(8, 8, 2, 4), (*SP, "tp"))
    placed = (P(SP, None), P(SP, "tp"), P(SP, "tp"), P(SP, "tp"), P("tp", SP))
    return jax.shard_map(
        on_device, mesh=grid, in_specs=placed, out_specs=P((*SP, "tp"), None), check_vma=False
    )
```

```python
import jax
import jax.numpy as jnp
from jax import lax
from jax.experimental import pallas as pl
from jax.experimental.pallas import tpu as pltpu
from jax.sharding import Mesh
from jax.sharding import PartitionSpec as P

DH = 128
ROWS = 512
ROPE_BASE = 500000.0
SP = ("z", "y", "core")
F32 = jnp.float32
BF16 = jnp.bfloat16
SCALE = DH ** (-0.5)
MIB = 1024 * 1024


def spread(value, axis):
    copies = jnp.broadcast_to(value, (lax.axis_size(axis), *value.shape))
    return lax.all_to_all(copies, axis, split_axis=0, concat_axis=0, tiled=True)


def from_behind(block, distance):
    size = lax.axis_size(SP)
    return lax.ppermute(block, SP, [(i - distance, i) for i in range(distance, size)])


def from_partner(block):
    return lax.ppermute(block, "core", [(0, 1), (1, 0)])


def pinned(value):
    return pltpu.with_memory_space_constraint(value, pltpu.HBM)


def call(body, outs, scratch=(), flops=0, moved=0, name=None, in_specs=None):
    extra = {} if in_specs is None else {"in_specs": in_specs}
    return pl.pallas_call(
        body,
        out_shape=outs,
        scratch_shapes=list(scratch),
        compiler_params=pltpu.CompilerParams(vmem_limit_bytes=16 * MIB),
        cost_estimate=pl.CostEstimate(flops=flops, bytes_accessed=moved, transcendentals=0),
        name=name,
        **extra,
    )


def tables(offset):
    positions = (offset + jnp.arange(ROWS, dtype=jnp.int32)).astype(F32)
    frequency = 1.0 / ROPE_BASE ** (jnp.arange(0, DH, 2, dtype=F32) / DH)
    angles = positions[:, None] * frequency[None, :]
    cosine, sine = jnp.cos(angles), jnp.sin(angles)
    return jnp.concatenate([cosine, cosine], axis=1), jnp.concatenate([-sine, sine], axis=1)


def turned(raw, cos_ref, sin_ref):
    return raw * cos_ref[...] + pltpu.roll(raw, DH // 2, 1) * sin_ref[...]


def reorder_body(tok_ref, out_ref):
    row = lax.broadcasted_iota(jnp.int32, (256, 256), 0)
    col = lax.broadcasted_iota(jnp.int32, (256, 256), 1)
    target = ((row >> 4) & 1) * 128 + (row >> 5) * 16 + (row & 15)
    moves = (col == target).astype(BF16)
    for z in range(8):
        part = tok_ref[:, z * 256 : (z + 1) * 256]
        out_ref[:, z * 256 : (z + 1) * 256] = jnp.dot(part, moves, preferred_element_type=F32).astype(BF16)


def pack_body(q_hbm, k_hbm, v_hbm, o_hbm, out_ref, q_ref, k_ref, v_ref, o_ref, sem):
    copies = [
        pltpu.make_async_copy(source, target, sem.at[i])
        for i, (source, target) in enumerate(
            ((q_hbm, q_ref), (k_hbm, k_ref), (v_hbm, v_ref), (o_hbm, o_ref))
        )
    ]
    for copy in copies:
        copy.start()
    for copy in copies:
        copy.wait()
    for y in range(8):
        out_ref[y, :, 0:256] = k_ref[:, :256]
        out_ref[y, :, 256:512] = v_ref[:, :256]
        out_ref[y, :, 512:640] = o_ref[...]
        out_ref[y, :, 640:1024] = q_ref[...]
        out_ref[y, :, 1024:1152] = k_ref[:, 256:]
        out_ref[y, :, 1152:1280] = v_ref[:, 256:]


def unpack_body(line_ref, most_ref, third_ref):
    for y in range(8):
        at = slice(y * 16, (y + 1) * 16)
        most_ref[at] = line_ref[y, :, :1024]
        for z in range(8):
            third_ref[z, at] = line_ref[y, :, 1024:]


def by_residue(value, stage_ref, out_ref, base, stride):
    stage_ref[...] = value
    count = ROWS // stride
    for r in range(stride):
        out_ref[base + r * count : base + (r + 1) * count, :] = stage_ref[
            pl.ds(r, count, stride=stride), :
        ].astype(BF16)


def kv3_body(tok_ref, w_ref, cos_ref, sin_ref, out_ref, stage_ref):
    acc = jnp.zeros((ROWS, 2 * DH), F32)
    for z in range(8):
        rows = jnp.concatenate([w_ref[0, z], w_ref[1, z]], axis=0)
        acc = acc + jnp.dot(tok_ref[:, z * 256 : (z + 1) * 256], rows, preferred_element_type=F32)
    by_residue(turned(acc[:, :DH], cos_ref, sin_ref), stage_ref, out_ref, 0, 16)
    by_residue(acc[:, DH:], stage_ref, out_ref, ROWS, 16)


def kv12_body(tok_ref, plane_ref, cos_ref, sin_ref, own_ref, send_ref, stage_ref, w_ref, key_sem, value_sem):
    key_copy = pltpu.make_async_copy(plane_ref.at[:, : 2 * DH], w_ref.at[:, : 2 * DH], key_sem)
    value_copy = pltpu.make_async_copy(plane_ref.at[:, 2 * DH : 4 * DH], w_ref.at[:, 2 * DH :], value_sem)
    key_copy.start()
    value_copy.start()
    key_copy.wait()
    keys = jnp.dot(tok_ref[...], w_ref[:, : 2 * DH], preferred_element_type=F32)
    near = turned(keys[:, :DH], cos_ref, sin_ref).astype(BF16)
    own_ref[:ROWS] = near
    send_ref[:128] = near[ROWS - 128 :]
    by_residue(turned(keys[:, DH:], cos_ref, sin_ref), stage_ref, send_ref, 256, 4)
    value_copy.wait()
    values = jnp.dot(tok_ref[...], w_ref[:, 2 * DH :], preferred_element_type=F32)
    near = values[:, :DH].astype(BF16)
    own_ref[ROWS:] = near
    send_ref[128:256] = near[ROWS - 128 :]
    by_residue(values[:, DH:], stage_ref, send_ref, 256 + ROWS, 4)


def product(query, key):
    return lax.dot_general(query, key, (((1,), (1,)), ((), ())), preferred_element_type=F32)


def shares(scores, allowed):
    scores = jnp.where(allowed, scores * SCALE, -jnp.inf)
    top = jnp.max(scores, axis=-1, keepdims=True)
    weight = jnp.exp(scores - top)
    total = jnp.sum(weight, axis=-1, keepdims=True)
    return (weight * (1.0 / total)).astype(BF16), top + jnp.log(total)


def attend(query, key, value, allowed):
    probs, log_total = shares(product(query, key), allowed)
    return jnp.dot(probs, value, preferred_element_type=F32), log_total


def q_body(tok_ref, plane_ref, cos_ref, sin_ref, q_ref, stage_ref, w_ref, first_sem, third_sem):
    first_copy = pltpu.make_async_copy(plane_ref.at[:, 640:896], w_ref.at[:, :256], first_sem)
    third_copy = pltpu.make_async_copy(plane_ref.at[:, 896:1024], w_ref.at[:, 256:], third_sem)
    first_copy.start()
    third_copy.start()
    first_copy.wait()
    first = jnp.dot(tok_ref[...], w_ref[:, :256], preferred_element_type=F32)
    q_ref[:ROWS] = turned(first[:, :DH], cos_ref, sin_ref).astype(BF16)
    by_residue(turned(first[:, DH:], cos_ref, sin_ref), stage_ref, q_ref, ROWS, 4)
    third_copy.wait()
    third = jnp.dot(tok_ref[...], w_ref[:, 256:], preferred_element_type=F32)
    by_residue(turned(third, cos_ref, sin_ref), stage_ref, q_ref, 2 * ROWS, 16)


def near_body(spi_ref, q_ref, own_ref, send_ref, halo_ref, out_ref, log_ref, out2, log2):
    spi = spi_ref[0, 0]
    row = lax.broadcasted_iota(jnp.int32, (128, 256), 0)
    col = lax.broadcasted_iota(jnp.int32, (128, 256), 1)
    back = row + 128 - col
    inside = (back >= 0) & (back <= 128)
    edge = inside & ((col >= 128) | (spi >= 1))
    for r in range(4):
        at = slice(256 + r * 128, 256 + (r + 1) * 128)
        later = slice(256 + ROWS + r * 128, 256 + ROWS + (r + 1) * 128)
        key = jnp.concatenate([halo_ref[at], send_ref[at]], axis=0)
        value = jnp.concatenate([halo_ref[later], send_ref[later]], axis=0)
        out, log_total = attend(q_ref[ROWS + r * 128 : ROWS + (r + 1) * 128], key, value, edge)
        out2[pl.ds(r, 128, stride=4), :] = out
        log2[pl.ds(r, 128, stride=4), :] = jnp.broadcast_to(log_total, (128, DH))
    for b in range(4):
        if b == 0:
            key = jnp.concatenate([halo_ref[:128], own_ref[:128]], axis=0)
            value = jnp.concatenate([halo_ref[128:256], own_ref[ROWS : ROWS + 128]], axis=0)
        else:
            key = own_ref[(b - 1) * 128 : (b + 1) * 128]
            value = own_ref[ROWS + (b - 1) * 128 : ROWS + (b + 1) * 128]
        at = slice(b * 128, (b + 1) * 128)
        out, log_total = attend(q_ref[at], key, value, edge if b == 0 else inside)
        out_ref[at] = out
        log_ref[at] = jnp.broadcast_to(log_total, (128, DH))
    for b in range(4):
        at = slice(b * 128, (b + 1) * 128)
        out_ref[at], log_ref[at] = joined(out_ref[at], log_ref[at], out2[at], log2[at])


def joined(one, log_one, two, log_two):
    top = jnp.maximum(log_one, log_two)
    e1, e2 = jnp.exp(log_one - top), jnp.exp(log_two - top)
    total = e1 + e2
    return (e1 * one + e2 * two) / total, top + jnp.log(total)


def far_body(spi_ref, q_ref, x4, x3, x2, x1, x0, near_ref, near_log_ref, merged_ref, out3, log3):
    spi = spi_ref[0, 0]
    row = lax.broadcasted_iota(jnp.int32, (ROWS, 160), 0) & 31
    col = lax.broadcasted_iota(jnp.int32, (ROWS, 160), 1)
    back = row + 128 - col
    allowed = (back >= 0) & (back <= 128) & ((col >> 5) + spi >= 4)
    scores = []
    for r in range(16):
        at = slice(r * 32, (r + 1) * 32)
        key = jnp.concatenate([x[at] for x in (x4, x3, x2, x1, x0)], axis=0)
        scores.append(product(q_ref[2 * ROWS + r * 32 : 2 * ROWS + (r + 1) * 32], key))
    probs, log_total = shares(jnp.concatenate(scores, axis=0), allowed)
    wide = jnp.broadcast_to(log_total, (ROWS, DH))
    outs = []
    for r in range(16):
        later = slice(ROWS + r * 32, ROWS + (r + 1) * 32)
        value = jnp.concatenate([x[later] for x in (x4, x3, x2, x1, x0)], axis=0)
        outs.append(jnp.dot(probs[r * 32 : (r + 1) * 32], value, preferred_element_type=F32))
    for r in range(16):
        out3[pl.ds(r, 32, stride=16), :] = outs[r]
        log3[pl.ds(r, 32, stride=16), :] = wide[r * 32 : (r + 1) * 32]
    for b in range(4):
        at = slice(b * 128, (b + 1) * 128)
        merged, _ = joined(near_ref[at], near_log_ref[at], out3[at], log3[at])
        merged_ref[at] = merged.astype(BF16)


def out_body(tp_ref, m_ref, own_ref, below_ref, above_ref, across_low_ref, across_high_ref, out_ref):
    tp = tp_ref[0, 0]
    pair_a = jnp.concatenate([m_ref[tp], m_ref[(tp + 3) & 3]], axis=1)
    pair_b = jnp.concatenate([m_ref[(tp + 1) & 3], m_ref[(tp + 2) & 3]], axis=1)
    for z in range(8):
        starts = [z * 256 + c * 128 + y * 16 for y in range(8) for c in range(2)]
        own, below, above = (
            jnp.concatenate([ref[at : at + 16, :] for at in starts], axis=0)
            for ref in (own_ref, below_ref, above_ref)
        )
        half, base = (across_low_ref, 0) if z < 4 else (across_high_ref, 1024)
        across = jnp.concatenate([half[at - base : at - base + 16, :] for at in starts], axis=0)
        out_ref[:, z * 256 : (z + 1) * 256] = (
            product(pair_a, jnp.concatenate([own, below], axis=1))
            + product(pair_b, jnp.concatenate([above, across], axis=1))
        ).astype(BF16)


def shape(rows, cols, dtype=BF16):
    return jax.ShapeDtypeStruct((rows, cols), dtype)


def on_device(tokens, w_query, w_key, w_value, w_out):
    spi = lax.axis_index(SP).astype(jnp.int32)
    core = lax.axis_index("core")
    vmem = pl.BlockSpec(memory_space=pltpu.VMEM)
    smem = pl.BlockSpec(memory_space=pltpu.SMEM)
    anywhere = pl.BlockSpec(memory_space=pltpu.HBM)
    dma = pltpu.SemaphoreType.DMA
    stage = pltpu.VMEM((ROWS, DH), F32)

    packed = call(
        pack_body,
        jax.ShapeDtypeStruct((8, 16, 1280), BF16),
        [pltpu.VMEM((16, 384), BF16)] * 3 + [pltpu.VMEM((16, DH), BF16), pltpu.SemaphoreType.DMA((4,))],
        moved=MIB,
        name="pack",
        in_specs=[anywhere] * 4,
    )(pinned(w_query), pinned(w_key), pinned(w_value), pinned(w_out.T))
    line = lax.all_to_all(packed, "y", split_axis=0, concat_axis=0, tiled=True)
    most, third = call(
        unpack_body, (shape(128, 1024), jax.ShapeDtypeStruct((8, 128, 256), BF16)), moved=MIB, name="unpack"
    )(line)
    plane = lax.all_gather(most, ("z", "core"), axis=0, tiled=True)
    third = spread(lax.all_to_all(third, "z", split_axis=0, concat_axis=0, tiled=True), "core")

    cos, sin = tables(spi * ROWS)
    tok = call(reorder_body, shape(ROWS, 2048), flops=2 * ROWS * 2048 * 256, moved=4 * MIB, name="reorder")(tokens)

    x0 = call(
        kv3_body, shape(2 * ROWS, DH), [stage], 2 * ROWS * 2048 * 256, 4 * MIB, "kv3"
    )(tok, third, cos, sin)
    x2 = from_behind(x0, 2)
    kept, x2 = lax.optimization_barrier((jnp.where(core == 0, x0, x2), x2))
    x4 = from_behind(x2, 2)
    x1 = from_partner(kept)

    wo = plane[:, 512:640]
    below = lax.ppermute(wo, "tp", [(i, (i + 1) % 4) for i in range(4)])
    above = lax.ppermute(wo, "tp", [(i, (i + 3) % 4) for i in range(4)])
    own, send = call(
        kv12_body,
        (shape(2 * ROWS, DH), shape(1280, DH)),
        [stage, pltpu.VMEM((2048, 512), BF16), dma, dma],
        2 * ROWS * 2048 * 512,
        5 * MIB,
        "kv12",
        [vmem, anywhere, vmem, vmem],
    )(tok, pinned(plane), cos, sin)
    wo = plane[:, 512:640]
    below = lax.ppermute(wo, "tp", [(i, (i + 1) % 4) for i in range(4)])
    above = lax.ppermute(wo, "tp", [(i, (i + 3) % 4) for i in range(4)])
    tok_after, send = lax.optimization_barrier((tok, send))
    halo = from_behind(send, 1)
    queries = call(
        q_body,
        shape(3 * ROWS, DH),
        [stage, pltpu.VMEM((2048, 384), BF16), dma, dma],
        2 * ROWS * 2048 * 384,
        4 * MIB,
        "q",
        [vmem, anywhere, vmem, vmem],
    )(tok_after, pinned(plane), cos, sin)
    x4, queries = lax.optimization_barrier((x4, queries))
    x3 = from_partner(jnp.where(core == 0, x2, x4))
    spi_cell = spi.reshape(1, 1)
    near, near_log = call(
        near_body,
        (shape(ROWS, DH, F32), shape(ROWS, DH, F32)),
        [stage] * 2,
        8 * 4 * 128 * 256 * 128,
        2 * MIB,
        "near",
        [smem] + [vmem] * 4,
    )(spi_cell, queries, own, send, halo)
    merged = call(
        far_body,
        shape(ROWS, DH),
        [stage] * 2,
        4 * 512 * 256 * 128,
        3 * MIB,
        "far",
        [smem] + [vmem] * 8,
    )(spi_cell, queries, x4, x3, x2, x1, x0, near, near_log)
    merged, low, high = lax.optimization_barrier((merged, below[:1024], above[1024:]))
    across_low = lax.ppermute(low, "tp", [(i, (i + 1) % 4) for i in range(4)])
    across_high = lax.ppermute(high, "tp", [(i, (i + 3) % 4) for i in range(4)])
    by_position = lax.all_to_all(merged.reshape(4, 128, DH), "tp", split_axis=0, concat_axis=0, tiled=True)
    return call(
        out_body,
        shape(128, 2048),
        flops=2 * 128 * 512 * 2048,
        moved=3 * MIB,
        name="project",
        in_specs=[smem] + [vmem] * 6,
    )(lax.axis_index("tp").astype(jnp.int32).reshape(1, 1), by_position, wo, below, above, across_low, across_high)


def solution(mesh):
    grid = Mesh(mesh.devices.reshape(8, 8, 2, 4), (*SP, "tp"))
    placed = (P(SP, None), P(SP, "tp"), P(SP, "tp"), P(SP, "tp"), P("tp", SP))
    return jax.shard_map(
        on_device, mesh=grid, in_specs=placed, out_specs=P((*SP, "tp"), None), check_vma=False
    )
```
